32 devices in a mesh: rep: 2 (over x), fs: 8 (over z, y), tp: 2 (over core).
Axes of the slice: x: 2, y: 2, z: 4, core: 2. Of those that a mesh axis runs over, the one named last changes fastest.
Arguments:
- tokens: bfloat16 [8192, 2048], P(('rep', 'fs'), 'tp'), may hold values from -6 to 6
- mix_gain: float32 [2048], replicated, may hold values from 0.1 to 1.9
- query_w: bfloat16 [2048, 2048], P('fs', 'tp'), may hold values from -0.125 to 0.125
- key_w: bfloat16 [2048, 2048], P('fs', 'tp'), may hold values from -0.125 to 0.125
- value_w: bfloat16 [2048, 4096], P('fs', 'tp'), may hold values from -0.125 to 0.125
- head_gain: float32 [8, 512], replicated, may hold values from 0.1 to 1.9
- out_w: bfloat16 [4096, 2048], P('tp', 'fs'), may hold values from -0.09375 to 0.09375
- chan_gain: float32 [2048], replicated, may hold values from 0.1 to 1.9
- up_w: bfloat16 [2048, 4096], P('fs', 'tp'), may hold values from -0.125 to 0.125
- down_w: bfloat16 [4096, 2048], P('tp', 'fs'), may hold values from -0.09375 to 0.09375
Outputs:
- layer_out: bfloat16 [8192, 2048], P(('rep', 'fs'), 'tp')
The draws below stay inside these ranges and needn't reach their ends.
All inputs are finite; a program needn't handle non-finite values.
Results may differ from the reference program's by a relative error of at most 0.019.
Values may be sent and summed in bfloat16 or wider, within the bound.
No kernel may reach another device: no remote copies, remote signals or barrier semaphores. Data moves between devices by JAX's collectives and lax.ppermute only.
A program may use at most 128 MiB of HBM per device.

```python
import jax
import jax.numpy as jnp
from jax import lax

D = 2048
HEADS = 8
DK = 256
DV = 512
FF = 4096
BLOCK = 128
TOK = 512
TOKENS = 8192
N_TP = 2


def block_scale(key, dims, shards, low, high):
    def one(dim, blocks):
        draws = jax.random.uniform(jax.random.fold_in(jax.random.fold_in(key, 6), dim), (blocks,), jnp.float32, low / len(shards), high / len(shards))
        return jnp.repeat(jnp.exp(draws), dims[dim] // blocks).reshape((-1,) + (1,) * (len(dims) - dim - 1))

    level = one(*shards[0])
    for cut in shards[1:]:
        level = level * one(*cut)
    return level


def noise(stream_key, shape, deviation, bound, shards=(), kind=jnp.bfloat16):
    values = jax.random.normal(stream_key, shape, jnp.float32) * deviation
    if len(shards) > 0:
        values = block_scale(stream_key, shape, shards, -0.22, 0.18) * values
    return jnp.clip(values, min=-bound, max=bound).astype(kind)


def setup_inputs(seed: int = 0) -> dict:
    splits = jax.random.split(jax.random.key(seed), 11)
    return {
        "tokens": noise(splits[0], (TOKENS, D), 1.0, 6.0, ((0, 16), (1, 2))),
        "mix_gain": jnp.clip(1.0 + 0.18 * jax.random.normal(splits[1], (D,), jnp.float32), 0.1, 1.9),
        "query_w": noise(splits[2], (D, D), D ** -0.5, 0.125, ((0, 8), (1, 2))),
        "key_w": noise(splits[3], (D, D), D ** -0.5, 0.125, ((0, 8), (1, 2))),
        "value_w": noise(splits[4], (D, HEADS * DV), D ** -0.5, 0.125, ((0, 8), (1, 2))),
        "head_gain": jnp.clip(1.0 + 0.18 * jax.random.normal(splits[5], (HEADS, DV), jnp.float32), 0.1, 1.9),
        "out_w": noise(splits[6], (HEADS * DV, D), (HEADS * DV) ** -0.5, 0.09375, ((0, 2), (1, 8))),
        "chan_gain": jnp.clip(1.0 + 0.18 * jax.random.normal(splits[7], (D,), jnp.float32), 0.1, 1.9),
        "up_w": noise(splits[8], (D, FF), D ** -0.5, 0.125, ((0, 8), (1, 2))),
        "down_w": noise(splits[9], (FF, D), FF ** -0.5, 0.09375, ((0, 2), (1, 8))),
    }


EPS = 1e-06
HEAD_EPS = 0.05
THETA = 10000.0

def norm_rows(rows, gain):
    values = rows.astype(jnp.float32)
    scale = lax.rsqrt(lax.optimization_barrier(jnp.mean(values * values, axis=-1, keepdims=True)) + EPS)
    return (values * scale * gain).astype(jnp.bfloat16)

def rotate(field, places):
    half = field.shape[-1] // 2
    inverse = THETA ** (-jnp.arange(half, dtype=jnp.float32) / half)
    angles = places[:, None] * inverse
    cosine = jnp.cos(angles)[:, None, :]
    sine = jnp.sin(angles)[:, None, :]
    first = field[..., :half]
    second = field[..., half:]
    return jnp.concatenate([first * cosine - second * sine, second * cosine + first * sine], axis=-1)

def retain(query, keys, values, log_rate):
    count = query.shape[0] // BLOCK
    q_blocks = query.reshape(count, BLOCK, query.shape[1])
    k_blocks = keys.reshape(count, BLOCK, keys.shape[1])
    v_blocks = values.reshape(count, BLOCK, values.shape[1])
    place = jnp.arange(BLOCK, dtype=jnp.float32)
    offset = place[:, None] - place[None, :]
    mask = jnp.where(offset >= 0, jnp.exp(log_rate * jnp.maximum(offset, 0.0)), 0.0)
    q_decay = jnp.exp(log_rate * (place + 1.0))
    k_decay = jnp.exp(log_rate * (BLOCK - 1.0 - place))
    block_decay = jnp.exp(log_rate * BLOCK)

    def advance(state, item):
        q_part, k_part, v_part = item
        scores = jnp.dot(q_part, k_part.T, preferred_element_type=jnp.float32)
        weights = (scores * mask).astype(jnp.bfloat16)
        result = jnp.dot(weights, v_part, preferred_element_type=jnp.float32)
        q_scaled = (q_part.astype(jnp.float32) * q_decay[:, None]).astype(jnp.bfloat16)
        result = result + jnp.dot(q_scaled, state.astype(jnp.bfloat16), preferred_element_type=jnp.float32)
        k_scaled = (k_part.astype(jnp.float32) * k_decay[:, None]).astype(jnp.bfloat16)
        state = state * block_decay + jnp.dot(k_scaled.T, v_part, preferred_element_type=jnp.float32)
        return (state, result)
    start = jnp.zeros((query.shape[1], values.shape[1]), jnp.float32)
    _, outputs = lax.scan(advance, start, (q_blocks, k_blocks, v_blocks))
    return outputs.reshape(count * BLOCK, values.shape[1])

def grouped_sum(left, right):
    width = left.shape[1] // N_TP
    total = jnp.zeros((left.shape[0], right.shape[1]), jnp.float32)
    for group in range(N_TP):
        term = jnp.dot(left[:, group * width:(group + 1) * width], right[group * width:(group + 1) * width], preferred_element_type=jnp.float32).astype(jnp.bfloat16)
        term = lax.optimization_barrier(term)
        total = total + term.astype(jnp.float32)
    return total

def reference(tokens, mix_gain, query_w, key_w, value_w, head_gain, out_w, chan_gain, up_w, down_w):
    normed = norm_rows(tokens, mix_gain)
    qraw = jnp.dot(normed, query_w, preferred_element_type=jnp.float32)
    kraw = jnp.dot(normed, key_w, preferred_element_type=jnp.float32)
    vraw = jnp.dot(normed, value_w, preferred_element_type=jnp.float32)
    places = (jnp.arange(TOKENS, dtype=jnp.int32) % TOK).astype(jnp.float32)
    query = rotate(qraw.reshape(TOKENS, HEADS, DK), places).astype(jnp.bfloat16)
    keys = (rotate(kraw.reshape(TOKENS, HEADS, DK), places) * DK ** (-0.5)).astype(jnp.bfloat16)
    values = vraw.reshape(TOKENS, HEADS, DV).astype(jnp.bfloat16)
    heads = jnp.arange(HEADS, dtype=jnp.int32).astype(jnp.float32)
    log_rate = jnp.log1p(-jnp.exp2(-5.0 - heads))
    count = TOKENS // TOK
    per_head = jax.vmap(retain, in_axes=(1, 1, 1, 0), out_axes=1)

    def one_sequence(item):
        return per_head(item[0], item[1], item[2], log_rate)
    retained = lax.map(one_sequence, (query.reshape(count, TOK, HEADS, DK), keys.reshape(count, TOK, HEADS, DK), values.reshape(count, TOK, HEADS, DV)))
    retained = retained.reshape(TOKENS, HEADS, DV)
    scale = lax.rsqrt(lax.optimization_barrier(jnp.mean(retained * retained, axis=-1, keepdims=True)) + HEAD_EPS)
    head_out = (retained * scale * head_gain).astype(jnp.bfloat16).reshape(TOKENS, HEADS * DV)
    middle = (tokens.astype(jnp.float32) + grouped_sum(head_out, out_w)).astype(jnp.bfloat16)
    chan_normed = norm_rows(middle, chan_gain)
    upward = jnp.dot(chan_normed, up_w, preferred_element_type=jnp.float32)
    hidden = jnp.square(jax.nn.relu(upward)).astype(jnp.bfloat16)
    return (middle.astype(jnp.float32) + grouped_sum(hidden, down_w)).astype(jnp.bfloat16)
```

```python
import jax
import jax.numpy as jnp
from jax import lax
from jax.sharding import PartitionSpec as P

DK = 256
DV = 512

EPS = 1e-06
HEAD_EPS = 0.05
THETA = 10000.0


def norm_rows(rows, gain):
    values = rows.astype(jnp.float32)
    scale = lax.rsqrt(jnp.mean(values * values, axis=-1, keepdims=True) + EPS)
    return (values * scale * gain).astype(jnp.bfloat16)


def swap(x, axis):
    return lax.ppermute(x, axis, [(0, 1), (1, 0)])


def join(x, axis, size, dim):
    if size == 1:
        return x
    if size != 2:
        return lax.all_gather(x, axis, axis=dim, tiled=True)
    other = swap(x, axis)
    first = lax.axis_index(axis) == 0
    return jnp.concatenate(
        [jnp.where(first, x, other), jnp.where(first, other, x)], axis=dim
    )


def sum_parts(x, axis, size, dim):
    if size == 1:
        return x
    if size != 2:
        return lax.psum_scatter(
            x.astype(jnp.bfloat16), axis, scatter_dimension=dim, tiled=True
        ).astype(jnp.float32)
    part = x.shape[dim] // 2
    me = lax.axis_index(axis)
    away = lax.dynamic_slice_in_dim(x, (1 - me) * part, part, dim).astype(jnp.bfloat16)
    kept = lax.dynamic_slice_in_dim(x, me * part, part, dim)
    return kept + swap(away, axis).astype(jnp.float32)


def gather_fs(x, dim):
    return lax.all_gather(x, "fs", axis=dim, tiled=True)


def share(x, count, dim):
    if count == 1:
        return x
    part = x.shape[dim] // count
    return lax.dynamic_slice_in_dim(x, lax.axis_index("rep") * part, part, dim)


def rotate(field, cosine, sine):
    half = field.shape[-1] // 2
    first = field[:, :half]
    second = field[:, half:]
    return jnp.concatenate(
        [first * cosine - second * sine, second * cosine + first * sine], axis=-1
    )


def make(mesh):
    tp = mesh.shape["tp"]
    rep = mesh.shape["rep"]

    def shards(
        tokens, mix_gain, query_w, key_w, value_w, head_gain, out_w, chan_gain, up_w, down_w
    ):
        rows = tokens.shape[0]
        local = query_w.shape[1] // DK
        pair = rep == 2
        split_heads = 2 if pair and local % 2 == 0 else 1
        split_units = 2 if pair and up_w.shape[1] % 256 == 0 else 1
        heads = local // split_heads

        qkv_w = gather_fs(
            jnp.concatenate(
                [
                    share(query_w, split_heads, 1),
                    share(key_w, split_heads, 1),
                    share(value_w, split_heads, 1),
                ],
                axis=1,
            ),
            0,
        )
        out_full = gather_fs(share(out_w, split_heads, 0), 1)
        up_full = gather_fs(share(up_w, split_units, 1), 0)
        down_full = gather_fs(share(down_w, split_units, 0), 1)

        first_head = lax.axis_index("tp") * local
        if split_heads == 2:
            first_head = first_head + lax.axis_index("rep") * heads
        numbers = (first_head + jnp.arange(heads, dtype=jnp.int32)).astype(jnp.float32)
        log_rate = jnp.log1p(-jnp.exp2(-5.0 - numbers))
        gains = lax.dynamic_slice_in_dim(head_gain, first_head, heads, 0)

        places = jnp.arange(rows, dtype=jnp.int32).astype(jnp.float32)
        inverse = THETA ** (-jnp.arange(DK // 2, dtype=jnp.float32) / (DK // 2))
        angles = places[:, None] * inverse
        cosine, sine = jnp.cos(angles), jnp.sin(angles)
        offset = places[:, None] - places[None, :]
        masks = [
            jnp.where(offset >= 0, jnp.exp(log_rate[h] * jnp.maximum(offset, 0.0)), 0.0)
            for h in range(heads)
        ]

        def mixer_terms(block):
            normed = norm_rows(join(block, "tp", tp, 1), mix_gain)
            raw = jnp.dot(normed, qkv_w, preferred_element_type=jnp.float32)
            outs = []
            for h in range(heads):
                query = rotate(raw[:, h * DK : (h + 1) * DK], cosine, sine).astype(jnp.bfloat16)
                at = heads * DK + h * DK
                keys = (rotate(raw[:, at : at + DK], cosine, sine) * DK ** (-0.5)).astype(
                    jnp.bfloat16
                )
                at = 2 * heads * DK + h * DV
                values = raw[:, at : at + DV].astype(jnp.bfloat16)
                scores = lax.dot_general(
                    query, keys, (((1,), (1,)), ((), ())), preferred_element_type=jnp.float32
                )
                weights = (scores * masks[h]).astype(jnp.bfloat16)
                kept = jnp.dot(weights, values, preferred_element_type=jnp.float32)
                scale = lax.rsqrt(jnp.mean(kept * kept, axis=-1, keepdims=True) + HEAD_EPS)
                outs.append((kept * scale * gains[h]).astype(jnp.bfloat16))
            head_out = jnp.concatenate(outs, axis=1)
            terms = jnp.dot(head_out, out_full, preferred_element_type=jnp.float32)
            return sum_parts(terms, "tp", tp, 1)

        def chan_terms(block):
            normed = norm_rows(join(block, "tp", tp, 1), chan_gain)
            upward = jnp.dot(normed, up_full, preferred_element_type=jnp.float32)
            hidden = jnp.square(jax.nn.relu(upward)).astype(jnp.bfloat16)
            terms = jnp.dot(hidden, down_full, preferred_element_type=jnp.float32)
            return sum_parts(terms, "tp", tp, 1)

        def layer(block, terms, split):
            if split == 1:
                return (block.astype(jnp.float32) + terms(block)).astype(jnp.bfloat16)
            away = terms(swap(block, "rep")).astype(jnp.bfloat16)
            back = swap(away, "rep").astype(jnp.float32)
            return (block.astype(jnp.float32) + (terms(block) + back)).astype(jnp.bfloat16)

        middle = layer(tokens, mixer_terms, split_heads)
        return layer(middle, chan_terms, split_units)

    return shards


def solution(mesh):
    placed = (
        P(("rep", "fs"), "tp"),
        P(),
        P("fs", "tp"),
        P("fs", "tp"),
        P("fs", "tp"),
        P(),
        P("tp", "fs"),
        P(),
        P("fs", "tp"),
        P("tp", "fs"),
    )
    return jax.shard_map(
        make(mesh), mesh=mesh, in_specs=placed, out_specs=P(("rep", "fs"), "tp"), check_vma=False
    )
```

```python
import jax
import jax.numpy as jnp
from jax import lax
from jax.sharding import PartitionSpec as P


DK = 256
DV = 512

EPS = 1e-06
HEAD_EPS = 0.05
THETA = 10000.0


def norm_rows(block, gain, tp, width):
    if tp == 2:
        other = swap(block, "tp")
        first = lax.axis_index("tp") == 0
        halves = [jnp.where(first, block, other), jnp.where(first, other, block)]
        whole = [block, other]
    else:
        halves = [lax.all_gather(block, "tp", axis=1, tiled=True)]
        whole = halves
    total = sum(
        jnp.sum(jnp.square(part.astype(jnp.float32)), axis=-1, keepdims=True) for part in whole
    )
    scale = lax.rsqrt(total / gain.shape[0] + EPS)
    span = halves[0].shape[1]
    blocks = [half[:, at : at + width] for half in halves for at in range(0, span, width)]
    gains = [gain[at : at + width] for at in range(0, gain.shape[0], width)]
    return tuple(
        (rows.astype(jnp.float32) * scale * part).astype(jnp.bfloat16)
        for rows, part in zip(unweave(blocks), unweave(gains))
    )


def swap(x, axis):
    return lax.ppermute(x, axis, [(0, 1), (1, 0)])


def sum_parts(x, axis, size, dim):
    if size == 1:
        return x
    if size != 2:
        return lax.psum_scatter(
            x.astype(jnp.bfloat16), axis, scatter_dimension=dim, tiled=True
        ).astype(jnp.float32)
    part = x.shape[dim] // 2
    me = lax.axis_index(axis)
    away = lax.dynamic_slice_in_dim(x, (1 - me) * part, part, dim).astype(jnp.bfloat16)
    kept = lax.dynamic_slice_in_dim(x, me * part, part, dim)
    return kept + swap(away, axis).astype(jnp.float32)


def gather_fs(x, dim, size):
    groups = [list(range(0, size, 2)), list(range(1, size, 2))]
    return lax.all_gather(x, "fs", axis=dim, tiled=True, axis_index_groups=groups)


def cross(x, size):
    return lax.ppermute(x, "fs", [(i, i ^ 1) for i in range(size)])


def even():
    return lax.axis_index("fs") % 2 == 0


def unweave(blocks):
    mine = [jnp.where(even(), a, b) for a, b in zip(blocks[::2], blocks[1::2])]
    other = [jnp.where(even(), b, a) for a, b in zip(blocks[::2], blocks[1::2])]
    return jnp.concatenate(mine, axis=-1), jnp.concatenate(other, axis=-1)


def weave(mine, other, width):
    first = jnp.where(even(), mine, other)
    second = jnp.where(even(), other, mine)
    pieces = []
    for at in range(0, mine.shape[1], width):
        pieces += [first[:, at : at + width], second[:, at : at + width]]
    return jnp.concatenate(pieces, axis=1)


def share(x, count, dim):
    if count == 1:
        return x
    part = x.shape[dim] // count
    return lax.dynamic_slice_in_dim(x, lax.axis_index("rep") * part, part, dim)


def rotate(field, cosine, sine):
    half = field.shape[-1] // 2
    first = field[:, :half]
    second = field[:, half:]
    return jnp.concatenate(
        [first * cosine - second * sine, second * cosine + first * sine], axis=-1
    )


def make(mesh):
    tp = mesh.shape["tp"]
    rep = mesh.shape["rep"]
    fs = mesh.shape["fs"]

    def layer_body(
        tokens, mix_gain, query_w, key_w, value_w, head_gain, out_w, chan_gain, up_w, down_w
    ):
        rows = tokens.shape[0]
        local = query_w.shape[1] // DK
        pair = rep == 2
        split_heads = 2 if pair and local % 2 == 0 else 1
        split_units = 2 if pair and up_w.shape[1] % 256 == 0 else 1
        heads = local // split_heads

        width = query_w.shape[0]
        down_part = share(down_w, split_units, 0)
        down_other = cross(down_part, fs)
        qk_w = jnp.concatenate(
            [share(query_w, split_heads, 1), share(key_w, split_heads, 1)], axis=1
        )
        qk_mine = gather_fs(qk_w, 0, fs)
        value_mine = gather_fs(share(value_w, split_heads, 1), 0, fs)
        out_mine = gather_fs(share(out_w, split_heads, 0), 1, fs)
        up_mine = gather_fs(share(up_w, split_units, 1), 0, fs)
        down_full = gather_fs(weave(down_part, down_other, down_part.shape[1]), 1, fs)
        qk_other = cross(qk_mine, fs)
        value_other = cross(value_mine, fs)
        out_other = cross(out_mine, fs)
        up_other = cross(up_mine, fs)

        def product(rows, mine, other):
            return jnp.dot(rows[0], mine, preferred_element_type=jnp.float32) + jnp.dot(
                rows[1], other, preferred_element_type=jnp.float32
            )

        first_head = lax.axis_index("tp") * local
        if split_heads == 2:
            first_head = first_head + lax.axis_index("rep") * heads
        numbers = (first_head + jnp.arange(heads, dtype=jnp.int32)).astype(jnp.float32)
        log_rate = jnp.log1p(-jnp.exp2(-5.0 - numbers))
        gains = lax.dynamic_slice_in_dim(head_gain, first_head, heads, 0)

        places = jnp.arange(rows, dtype=jnp.int32).astype(jnp.float32)
        inverse = THETA ** (-jnp.arange(DK // 2, dtype=jnp.float32) / (DK // 2))
        angles = places[:, None] * inverse
        cosine, sine = jnp.cos(angles), jnp.sin(angles)
        offset = places[:, None] - places[None, :]
        masks = [
            jnp.where(offset >= 0, jnp.exp(log_rate[h] * jnp.maximum(offset, 0.0)), 0.0)
            for h in range(heads)
        ]

        def mixer_terms(block):
            normed = norm_rows(block, mix_gain, tp, width)
            raw = product(normed, qk_mine, qk_other)
            vraw = product(normed, value_mine, value_other).astype(jnp.bfloat16)
            outs = []
            for h in range(heads):
                query = rotate(raw[:, h * DK : (h + 1) * DK], cosine, sine).astype(jnp.bfloat16)
                at = heads * DK + h * DK
                keys = (rotate(raw[:, at : at + DK], cosine, sine) * DK ** (-0.5)).astype(
                    jnp.bfloat16
                )
                values = vraw[:, h * DV : (h + 1) * DV]
                scores = lax.dot_general(
                    query, keys, (((1,), (1,)), ((), ())), preferred_element_type=jnp.float32
                )
                weights = (scores * masks[h]).astype(jnp.bfloat16)
                kept = jnp.dot(weights, values, preferred_element_type=jnp.float32)
                scale = lax.rsqrt(jnp.mean(kept * kept, axis=-1, keepdims=True) + HEAD_EPS)
                outs.append((kept * scale * gains[h]).astype(jnp.bfloat16))
            head_out = jnp.concatenate(outs, axis=1)
            terms = [
                jnp.dot(head_out, part, preferred_element_type=jnp.float32)
                for part in (out_mine, out_other)
            ]
            if tp == 2 and (fs // tp) % 2 == 0:
                terms = [sum_parts(part, "tp", tp, 1) for part in terms]
                return terms
            return [sum_parts(weave(*terms, out_w.shape[1]), "tp", tp, 1)]

        def chan_terms(block):
            normed = norm_rows(block, chan_gain, tp, width)
            upward = product(normed, up_mine, up_other)
            hidden = jnp.square(jax.nn.relu(upward)).astype(jnp.bfloat16)
            terms = jnp.dot(hidden, down_full, preferred_element_type=jnp.float32)
            return [sum_parts(terms, "tp", tp, 1)]

        def layer(block, terms, split):
            if split == 1:
                total = terms(block)
            else:
                away = [part.astype(jnp.bfloat16) for part in terms(swap(block, "rep"))]
                back = [swap(part, "rep").astype(jnp.float32) for part in away]
                total = [part + more for part, more in zip(terms(block), back)]
            if len(total) == 2:
                total = [weave(*total, out_w.shape[1])]
            return (block.astype(jnp.float32) + total[0]).astype(jnp.bfloat16)

        middle = layer(tokens, mixer_terms, split_heads)
        return layer(middle, chan_terms, split_units)

    return layer_body


def solution(mesh):
    placed = (
        P(("rep", "fs"), "tp"),
        P(),
        P("fs", "tp"),
        P("fs", "tp"),
        P("fs", "tp"),
        P(),
        P("tp", "fs"),
        P(),
        P("fs", "tp"),
        P("tp", "fs"),
    )
    return jax.shard_map(
        make(mesh), mesh=mesh, in_specs=placed, out_specs=P(("rep", "fs"), "tp"), check_vma=False
    )
```

```python
import jax
import jax.numpy as jnp
from jax import lax
from jax.sharding import PartitionSpec as P


DK = 256
DV = 512

EPS = 1e-06
HEAD_EPS = 0.05
THETA = 10000.0


def norm_rows(block, gain, tp, width):
    if tp == 2:
        other = swap(block, "tp")
        first = lax.axis_index("tp") == 0
        halves = [jnp.where(first, block, other), jnp.where(first, other, block)]
        whole = [block, other]
    else:
        halves = [lax.all_gather(block, "tp", axis=1, tiled=True)]
        whole = halves
    total = sum(
        jnp.sum(jnp.square(part.astype(jnp.float32)), axis=-1, keepdims=True) for part in whole
    )
    scale = lax.rsqrt(total / gain.shape[0] + EPS)
    span = halves[0].shape[1]
    blocks = [half[:, at : at + width] for half in halves for at in range(0, span, width)]
    gains = [gain[at : at + width] for at in range(0, gain.shape[0], width)]
    return tuple(
        (rows.astype(jnp.float32) * scale * part).astype(jnp.bfloat16)
        for rows, part in zip(unweave(blocks), unweave(gains))
    )


def swap(x, axis):
    return lax.ppermute(x, axis, [(0, 1), (1, 0)])


def sum_parts(x, axis, size, dim):
    if size == 1:
        return x
    if size != 2:
        return lax.psum_scatter(
            x.astype(jnp.bfloat16), axis, scatter_dimension=dim, tiled=True
        ).astype(jnp.float32)
    part = x.shape[dim] // 2
    me = lax.axis_index(axis)
    away = lax.dynamic_slice_in_dim(x, (1 - me) * part, part, dim).astype(jnp.bfloat16)
    kept = lax.dynamic_slice_in_dim(x, me * part, part, dim)
    return kept + swap(away, axis).astype(jnp.float32)


def gather_fs(x, dim, size):
    groups = [list(range(0, size, 2)), list(range(1, size, 2))]
    return lax.all_gather(x, "fs", axis=dim, tiled=True, axis_index_groups=groups)


def cross(x, size):
    return lax.ppermute(x, "fs", [(i, i ^ 1) for i in range(size)])


def even():
    return lax.axis_index("fs") % 2 == 0


def unweave(blocks):
    mine = [jnp.where(even(), a, b) for a, b in zip(blocks[::2], blocks[1::2])]
    other = [jnp.where(even(), b, a) for a, b in zip(blocks[::2], blocks[1::2])]
    return jnp.concatenate(mine, axis=-1), jnp.concatenate(other, axis=-1)


def weave(mine, other, width):
    first = jnp.where(even(), mine, other)
    second = jnp.where(even(), other, mine)
    pieces = []
    for at in range(0, mine.shape[1], width):
        pieces += [first[:, at : at + width], second[:, at : at + width]]
    return jnp.concatenate(pieces, axis=1)


def share(x, count, dim):
    if count == 1:
        return x
    part = x.shape[dim] // count
    return lax.dynamic_slice_in_dim(x, lax.axis_index("rep") * part, part, dim)


def rotate(field, cosine, sine):
    half = field.shape[-1] // 2
    first = field[:, :half]
    second = field[:, half:]
    return jnp.concatenate(
        [first * cosine - second * sine, second * cosine + first * sine], axis=-1
    )


def make(mesh):
    tp = mesh.shape["tp"]
    rep = mesh.shape["rep"]
    fs = mesh.shape["fs"]

    def layer_body(
        tokens, mix_gain, query_w, key_w, value_w, head_gain, out_w, chan_gain, up_w, down_w
    ):
        rows = tokens.shape[0]
        local = query_w.shape[1] // DK
        pair = rep == 2
        split_heads = 2 if pair and local % 2 == 0 else 1
        split_units = 2 if pair and up_w.shape[1] % 256 == 0 else 1
        heads = local // split_heads

        width = query_w.shape[0]
        down_part = share(down_w, split_units, 0)
        down_other = cross(down_part, fs)
        qk_w = jnp.concatenate(
            [share(query_w, split_heads, 1), share(key_w, split_heads, 1)], axis=1
        )
        qk_mine = gather_fs(qk_w, 0, fs)
        value_mine = gather_fs(share(value_w, split_heads, 1), 0, fs)
        out_mine = gather_fs(share(out_w, split_heads, 0), 1, fs)
        up_mine = gather_fs(share(up_w, split_units, 1), 0, fs)
        down_full = gather_fs(weave(down_part, down_other, down_part.shape[1]), 1, fs)
        qk_other = cross(qk_mine, fs)
        value_other = cross(value_mine, fs)
        out_other = cross(out_mine, fs)
        up_other = cross(up_mine, fs)

        def product(rows, mine, other):
            return jnp.dot(rows[0], mine, preferred_element_type=jnp.float32) + jnp.dot(
                rows[1], other, preferred_element_type=jnp.float32
            )

        first_head = lax.axis_index("tp") * local
        if split_heads == 2:
            first_head = first_head + lax.axis_index("rep") * heads
        numbers = (first_head + jnp.arange(heads, dtype=jnp.int32)).astype(jnp.float32)
        log_rate = jnp.log1p(-jnp.exp2(-5.0 - numbers))
        gains = lax.dynamic_slice_in_dim(head_gain, first_head, heads, 0)

        places = jnp.arange(rows, dtype=jnp.int32).astype(jnp.float32)
        inverse = THETA ** (-jnp.arange(DK // 2, dtype=jnp.float32) / (DK // 2))
        angles = places[:, None] * inverse
        cosine, sine = jnp.cos(angles), jnp.sin(angles)
        offset = places[:, None] - places[None, :]
        masks = [
            jnp.where(offset >= 0, jnp.exp(log_rate[h] * jnp.maximum(offset, 0.0)), 0.0)
            for h in range(heads)
        ]

        def mixer_terms(block, after=None):
            normed = norm_rows(block, mix_gain, tp, width)
            raw = product(normed, qk_mine, qk_other)
            vraw = product(normed, value_mine, value_other).astype(jnp.bfloat16)
            outs = []
            for h in range(heads):
                query = rotate(raw[:, h * DK : (h + 1) * DK], cosine, sine).astype(jnp.bfloat16)
                at = heads * DK + h * DK
                keys = (rotate(raw[:, at : at + DK], cosine, sine) * DK ** (-0.5)).astype(
                    jnp.bfloat16
                )
                values = vraw[:, h * DV : (h + 1) * DV]
                scores = lax.dot_general(
                    query, keys, (((1,), (1,)), ((), ())), preferred_element_type=jnp.float32
                )
                weights = (scores * masks[h]).astype(jnp.bfloat16)
                kept = jnp.dot(weights, values, preferred_element_type=jnp.float32)
                scale = lax.rsqrt(jnp.mean(kept * kept, axis=-1, keepdims=True) + HEAD_EPS)
                outs.append((kept * scale * gains[h]).astype(jnp.bfloat16))
            head_out = jnp.concatenate(outs, axis=1)
            terms = [
                jnp.dot(head_out, part, preferred_element_type=jnp.float32)
                for part in (out_mine, out_other)
            ]
            if tp == 2 and (fs // tp) % 2 == 0:
                terms = [sum_parts(part, "tp", tp, 1) for part in terms]
                return terms
            return [sum_parts(weave(*terms, out_w.shape[1]), "tp", tp, 1)]

        def chan_terms(block, after=None):
            normed = norm_rows(block, chan_gain, tp, width)
            upward = product(normed, up_mine, up_other)
            hidden = jnp.square(jax.nn.relu(upward)).astype(jnp.bfloat16)
            if after is not None:
                hidden, after = lax.optimization_barrier((hidden, after))
            terms = jnp.dot(hidden, down_full, preferred_element_type=jnp.float32)
            return [sum_parts(terms, "tp", tp, 1)]

        def layer(block, terms, split):
            if split == 1:
                total = terms(block)
            else:
                away = [part.astype(jnp.bfloat16) for part in terms(swap(block, "rep"))]
                back = [swap(part, "rep").astype(jnp.float32) for part in away]
                total = [part + more for part, more in zip(terms(block, away[0]), back)]
            if len(total) == 2:
                total = [weave(*total, out_w.shape[1])]
            return (block.astype(jnp.float32) + total[0]).astype(jnp.bfloat16)

        middle = layer(tokens, mixer_terms, split_heads)
        return layer(middle, chan_terms, split_units)

    return layer_body


def solution(mesh):
    placed = (
        P(("rep", "fs"), "tp"),
        P(),
        P("fs", "tp"),
        P("fs", "tp"),
        P("fs", "tp"),
        P(),
        P("tp", "fs"),
        P(),
        P("fs", "tp"),
        P("tp", "fs"),
    )
    return jax.shard_map(
        make(mesh), mesh=mesh, in_specs=placed, out_specs=P(("rep", "fs"), "tp"), check_vma=False
    )
```
